32 devices in a mesh: kv: 8 (over z, y), tp: 4 (over x, core).
Axes of the slice: x: 2, y: 2, z: 4, core: 2. Of those that a mesh axis runs over, the one named last changes fastest.
Arguments:
- queries: bfloat16 [2048, 3072], P('kv', 'tp'), may hold values from -6 to 6
- key_vectors: bfloat16 [2048, 512], P('kv', 'tp'), may hold values from -6 to 6
- value_vectors: bfloat16 [2048, 512], P('kv', 'tp'), may hold values from -6 to 6
- log_sums: float32 [2048, 48], P('kv', 'tp'), may hold values from 4.5 to 6.5
- out_grad: bfloat16 [2048, 3072], P('kv', 'tp'), may hold values from -48 to 48
- layer_input: bfloat16 [2048, 3072], P('kv', 'tp'), may hold values from -0.29882812 to 0.29882812
- chosen: int32 [32, 16], P('kv'), may hold values from -1 to 55, as said below
Outputs:
- query_grad: bfloat16 [2048, 3072], P('kv', 'tp')
- key_grad: bfloat16 [2048, 512], P('kv', 'tp')
- value_grad: bfloat16 [2048, 512], P('kv', 'tp')
- weight_grad: float32 [3072, 512], P('kv', 'tp')
The draws below stay inside these ranges and needn't reach their ends.
Inputs may be any that keep to these rules, and one draw needn't show every extreme that they name: `chosen`: each entry is -1 or the number c of a block of 32 positions (c * 32 to c * 32 + 31) that lies wholly within an earlier index of kv than its query block. The numbers of one row differ, and all query blocks held by one index of kv together take at most one block from each other index.
All inputs are finite; a program needn't handle non-finite values.
Results may differ from the reference program's by a relative error of at most 0.0061.
Values may be sent and summed in bfloat16 or wider, within the bound.
No kernel may reach another device: no remote copies, remote signals or barrier semaphores. Data moves between devices by JAX's collectives and lax.ppermute only.
A program may use at most 64 MiB of HBM per device.

```python
import jax
import jax.numpy as jnp
from jax import lax

D = 3072
HEADS = 48
KV_HEADS = 8
HEAD = 64
KB = 32
QB = 64
NSEL = 16
TOK_DEV = 256
TOKENS = 2048
N_KV = 8


def draw_chosen(key, part):
    query_blocks = TOK_DEV // QB
    blocks_here = TOK_DEV // KB
    columns_all = N_KV + NSEL
    subkeys = jax.random.split(key, 5)
    device = jnp.arange(N_KV, dtype=jnp.int32)[:, None, None]
    owner_id = jnp.arange(columns_all, dtype=jnp.int32)[None, None, :]
    random_base = jax.random.randint(subkeys[0], (N_KV, query_blocks, columns_all), 0, 1 << 20)
    favour = jax.random.randint(subkeys[1], (N_KV, query_blocks, columns_all), 0, 4)
    wrap_pick = (owner_id == 0) & (device == N_KV - 1)
    forced = ((owner_id == device - 1) | (owner_id == device - N_KV // 2) | wrap_pick).astype(jnp.int32)
    ranking = ((favour + 8 * forced) * (1 << 20) + random_base) * columns_all + owner_id
    ranking = jnp.where(owner_id < device, ranking, -1 - owner_id)
    top_scores, top_owner = lax.top_k(ranking, NSEL)
    counts = jax.random.randint(subkeys[2], (N_KV, query_blocks, 1), max(3, NSEL // 2), NSEL + 1)
    slot_ids = jnp.arange(NSEL, dtype=jnp.int32)[None, None, :]
    live_slot = (top_scores >= 0) & (slot_ids < counts)
    block_pick = jax.random.randint(subkeys[3], (N_KV, columns_all), 0, blocks_here)
    upper_pick = jax.random.randint(subkeys[4], (N_KV, columns_all), 1, blocks_here)
    wrap_flat = (jnp.arange(columns_all, dtype=jnp.int32)[None, :] == 0) & (jnp.arange(N_KV, dtype=jnp.int32)[:, None] == N_KV - 1)
    block_pick = jnp.where(wrap_flat, upper_pick, block_pick)
    spread_pick = jnp.broadcast_to(block_pick[:, None, :], (N_KV, query_blocks, columns_all))
    picked = jnp.take_along_axis(spread_pick, top_owner, axis=2)
    entries = jnp.where(live_slot, top_owner * blocks_here + picked, -1)
    return entries.reshape(N_KV * query_blocks, NSEL).astype(jnp.int32)


def strengthened(result, stream_key, source, target, blocks, factor):
    def block_of(dim):
        return (jnp.arange(result.shape[dim]) // (result.shape[dim] // blocks)).reshape((-1,) + (1,) * (result.ndim - 1 - dim))

    near = jax.random.permutation(stream_key, blocks)[block_of(target)]
    second = (block_of(target) + blocks // 2) % blocks
    return jnp.where((block_of(source) == near) | (block_of(source) == second), factor * result, result)


def levels(key, dims, cuts, least, top_value):
    loudness = 1.0
    for axis_at, blocks in cuts:
        heights = jax.random.uniform(jax.random.fold_in(jax.random.fold_in(key, 6), axis_at), (blocks,), jnp.float32, least / len(cuts), top_value / len(cuts))
        loudness = loudness * jnp.repeat(jnp.exp(heights), dims[axis_at] // blocks).reshape((-1,) + (1,) * (len(dims) - 1 - axis_at))
    return loudness


def centred(key, dims, width, reach, cuts=(), held_as=jnp.bfloat16):
    gain = levels(key, dims, cuts, -0.22, 0.18) if cuts else 1.0
    values = jax.random.normal(key, dims, jnp.float32) * width * gain
    return jnp.minimum(jnp.maximum(values, -reach), reach).astype(held_as)


def gaussian_with(own_key, extent, scale, reach, pieces, heavy, kind=jnp.bfloat16):
    result = scale * jax.random.normal(own_key, extent, jnp.float32)
    if pieces:
        result = result * levels(own_key, extent, pieces, -0.22, 0.18)
    return jnp.clip(strengthened(result, jax.random.fold_in(own_key, 3), *heavy), -reach, reach).astype(kind)


def setup_inputs(seed: int = 0) -> dict:
    key_list = jax.random.split(jax.random.key(seed), 8)
    return {
        "queries": centred(key_list[0], (TOKENS, HEADS * HEAD), 1.0, 6.0, ((0, 8), (1, 4))),
        "key_vectors": centred(key_list[1], (TOKENS, KV_HEADS * HEAD), 1.0, 6.0, ((0, 8), (1, 4))),
        "value_vectors": centred(key_list[2], (TOKENS, KV_HEADS * HEAD), 1.0, 6.0, ((0, 8), (1, 4))),
        "log_sums": jnp.clip(4.5 + 2.0 * jax.random.uniform(key_list[3], (TOKENS, HEADS), jnp.float32) ** levels(key_list[3], (TOKENS, HEADS), ((0, 8), (1, 4)), -0.2, 0.2), 4.5, 6.5),
        "out_grad": centred(key_list[4], (TOKENS, HEADS * HEAD), 8.0, 48.0, ((0, 8), (1, 4))),
        "layer_input": gaussian_with(key_list[5], (TOKENS, D), 0.05, 0.29882812, ((0, 8), (1, 4)), (0, 1, 8, 2.0)),
        "chosen": draw_chosen(jax.random.fold_in(key_list[7], 71), 0),
    }


def rounded(values_in):
    return lax.optimization_barrier(values_in.astype(jnp.bfloat16)).astype(jnp.float32)


def reference(queries, key_vectors, value_vectors, log_sums, out_grad, layer_input, chosen):
    group_size = HEADS // KV_HEADS
    score_scale = HEAD ** -0.5
    query_all = queries.reshape(TOKENS, KV_HEADS, group_size, HEAD)
    grad_all = out_grad.reshape(TOKENS, KV_HEADS, group_size, HEAD)
    sums_all = log_sums.reshape(TOKENS, KV_HEADS, group_size)
    key_all = key_vectors.reshape(TOKENS, KV_HEADS, HEAD)
    value_all = value_vectors.reshape(TOKENS, KV_HEADS, HEAD)
    block_offsets = jnp.arange(KB, dtype=jnp.int32)

    def block_step(accum, block_index):
        key_acc, value_acc = accum
        first_row = block_index * QB
        span_first = (first_row // TOK_DEV) * TOK_DEV
        query_rows = lax.dynamic_slice_in_dim(query_all, first_row, QB, 0).astype(jnp.float32)
        grad_rows = lax.dynamic_slice_in_dim(grad_all, first_row, QB, 0).astype(jnp.float32)
        sum_rows = lax.dynamic_slice_in_dim(sums_all, first_row, QB, 0)
        picks = chosen[block_index]
        usable = picks >= 0
        rows_sel = (jnp.maximum(picks, 0)[:, None] * KB + block_offsets[None, :]).reshape(-1)
        keep_key = jnp.repeat(usable, KB)
        key_sel = key_all[rows_sel].astype(jnp.float32)
        value_sel = value_all[rows_sel].astype(jnp.float32)
        key_own = lax.dynamic_slice_in_dim(key_all, span_first, TOK_DEV, 0).astype(jnp.float32)
        value_own = lax.dynamic_slice_in_dim(value_all, span_first, TOK_DEV, 0).astype(jnp.float32)
        query_pos = first_row + jnp.arange(QB, dtype=jnp.int32)
        key_pos = span_first + jnp.arange(TOK_DEV, dtype=jnp.int32)
        causal = key_pos[None, :] <= query_pos[:, None]
        score_sel = jnp.einsum("qhgd,khd->qhgk", query_rows, key_sel) * score_scale
        score_own = jnp.einsum("qhgd,khd->qhgk", query_rows, key_own) * score_scale
        weight_sel = jnp.where(keep_key[None, None, None, :], jnp.exp(score_sel - sum_rows[..., None]), 0.0)
        weight_own = jnp.where(causal[:, None, None, :], jnp.exp(score_own - sum_rows[..., None]), 0.0)
        round_sel = rounded(weight_sel)
        round_own = rounded(weight_own)
        output = jnp.einsum("qhgk,khd->qhgd", round_sel, value_sel) + jnp.einsum("qhgk,khd->qhgd", round_own, value_own)
        row_delta = jnp.sum(grad_rows * output, axis=-1)
        slope_sel = rounded(weight_sel * (jnp.einsum("qhgd,khd->qhgk", grad_rows, value_sel) - row_delta[..., None]))
        slope_own = rounded(weight_own * (jnp.einsum("qhgd,khd->qhgk", grad_rows, value_own) - row_delta[..., None]))
        query_grad = (jnp.einsum("qhgk,khd->qhgd", slope_sel, key_sel) + jnp.einsum("qhgk,khd->qhgd", slope_own, key_own)) * score_scale
        key_part = jnp.einsum("qhgk,qhgd->khd", slope_sel, query_rows) * score_scale
        value_part = jnp.einsum("qhgk,qhgd->khd", round_sel, grad_rows)
        key_own_part = jnp.einsum("qhgk,qhgd->khd", slope_own, query_rows) * score_scale
        value_own_part = jnp.einsum("qhgk,qhgd->khd", round_own, grad_rows)
        key_acc = key_acc.at[rows_sel].add(key_part)
        value_acc = value_acc.at[rows_sel].add(value_part)
        key_acc = lax.dynamic_update_slice_in_dim(key_acc, lax.dynamic_slice_in_dim(key_acc, span_first, TOK_DEV, 0) + key_own_part, span_first, 0)
        value_acc = lax.dynamic_update_slice_in_dim(value_acc, lax.dynamic_slice_in_dim(value_acc, span_first, TOK_DEV, 0) + value_own_part, span_first, 0)
        return (key_acc, value_acc), query_grad.astype(jnp.bfloat16)

    zeros_acc = jnp.zeros((TOKENS, KV_HEADS, HEAD), jnp.float32)
    (key_acc, value_acc), grads = lax.scan(block_step, (zeros_acc, zeros_acc), jnp.arange(TOKENS // QB, dtype=jnp.int32))
    query_grad = grads.reshape(TOKENS, HEADS * HEAD)
    key_grad = key_acc.reshape(TOKENS, KV_HEADS * HEAD).astype(jnp.bfloat16)
    value_grad = value_acc.reshape(TOKENS, KV_HEADS * HEAD).astype(jnp.bfloat16)
    weight_grad = jnp.dot(layer_input.T, key_grad, preferred_element_type=jnp.float32)
    return (query_grad, key_grad, value_grad, weight_grad)
```

```python
import math

import jax
import jax.numpy as jnp
from jax import lax
from jax.experimental import pallas as pl
from jax.experimental.pallas import tpu as pltpu
from jax.sharding import PartitionSpec as P

HEAD = 64
KB = 32
QB = 64
PAD_ROWS = 16
MASKED = -1e30


def dot_nt(a, b):
    return lax.dot_general(a, b, (((1,), (1,)), ((), ())), preferred_element_type=jnp.float32)


def dot_nn(a, b):
    return lax.dot_general(a, b, (((1,), (0,)), ((), ())), preferred_element_type=jnp.float32)


def dot_tn(a, b):
    return lax.dot_general(a, b, (((0,), (0,)), ((), ())), preferred_element_type=jnp.float32)


def attention_kernel(wanted, q_ref, g_ref, kv_ref, all_ref, sums_ref, bias_ref,
                     dq_ref, own_ref, sel_ref,
                     kv_sel, dk_own, dv_own, dk_sel, dv_sel, p_buf, dp_buf):
    span = q_ref.shape[0]
    half = kv_ref.shape[1] // 2
    kv_local = half // HEAD
    group = q_ref.shape[1] // half
    blocks = span // QB
    owners = all_ref.shape[0]
    scale = HEAD ** -0.5
    chunk = math.gcd(owners, 8) * KB
    chunks = owners * KB // chunk

    def fetch(o, carry):
        first = pl.multiple_of(jnp.maximum(wanted[o], 0) * KB, KB)
        kv_sel[pl.ds(pl.multiple_of(o * KB, KB), KB), :] = all_ref[o, pl.ds(first, KB), :]
        return carry

    if owners <= 8:
        for o in range(owners):
            fetch(o, 0)
    else:
        lax.fori_loop(0, owners, fetch, 0)

    def over_chunks(body, init):
        if chunks == 1:
            return body(0, init)
        return lax.fori_loop(0, chunks, body, init)

    key_id = lax.broadcasted_iota(jnp.int32, (QB, group * QB), 0)
    query_id = lax.broadcasted_iota(jnp.int32, (QB, group * QB), 1) % QB
    causal = key_id <= query_id

    for h in range(kv_local):
        k_lanes = slice(h * HEAD, (h + 1) * HEAD)
        v_lanes = slice(half + h * HEAD, half + (h + 1) * HEAD)
        for b in range(blocks):
            rows = slice(b * QB, (b + 1) * QB)
            heads = [h * group + i for i in range(group)]
            qs = jnp.concatenate([q_ref[rows, i * HEAD:(i + 1) * HEAD] for i in heads], axis=0)
            gs = jnp.concatenate([g_ref[rows, i * HEAD:(i + 1) * HEAD] for i in heads], axis=0)
            sums = sums_ref[h * blocks + b:h * blocks + b + 1, :]
            n_own = (b + 1) * QB
            k_own = kv_ref[:n_own, k_lanes]
            v_own = kv_ref[:n_own, v_lanes]
            p_own = jnp.exp(dot_nt(k_own, qs) * scale - sums)
            last = jnp.where(causal, p_own[b * QB:, :], 0.0)
            p_own = jnp.concatenate([p_own[:b * QB, :], last], axis=0) if b else last
            dp_own = dot_nt(v_own, gs)
            p16_own = p_own.astype(jnp.bfloat16)
            delta = jnp.sum(p16_own.astype(jnp.float32) * dp_own, axis=0, keepdims=True)

            def first_pass(c, delta):
                at = pl.ds(c * chunk, chunk)
                s = dot_nt(kv_sel[at, k_lanes], qs) * scale - sums
                p = jnp.exp(s + bias_ref[at, b:b + 1])
                dp = dot_nt(kv_sel[at, v_lanes], gs)
                p_buf[at, :] = p
                dp_buf[at, :] = dp
                p16 = p.astype(jnp.bfloat16)
                dv = dot_nn(p16, gs)
                dv_sel[h, at, :] = dv if b == 0 else dv_sel[h, at, :] + dv
                return delta + jnp.sum(p16.astype(jnp.float32) * dp, axis=0, keepdims=True)

            delta = over_chunks(first_pass, delta)
            ds_own = (p_own * (dp_own - delta)).astype(jnp.bfloat16)
            dqt = dot_tn(k_own, ds_own)
            dk = dot_nn(ds_own, qs)
            dv = dot_nn(p16_own, gs)
            if b:
                dk_own[h, :b * QB, :] += dk[:b * QB]
                dv_own[h, :b * QB, :] += dv[:b * QB]
            dk_own[h, b * QB:n_own, :] = dk[b * QB:]
            dv_own[h, b * QB:n_own, :] = dv[b * QB:]

            def second_pass(c, dqt):
                at = pl.ds(c * chunk, chunk)
                ds = (p_buf[at, :] * (dp_buf[at, :] - delta)).astype(jnp.bfloat16)
                dk = dot_nn(ds, qs)
                dk_sel[h, at, :] = dk if b == 0 else dk_sel[h, at, :] + dk
                return dqt + dot_tn(kv_sel[at, k_lanes], ds)

            dqt = over_chunks(second_pass, dqt)
            dq = (dqt * scale).T
            dq = jnp.concatenate([dq[i * QB:(i + 1) * QB] for i in range(group)], axis=1)
            dq_ref[rows, h * group * HEAD:(h + 1) * group * HEAD] = dq.astype(jnp.bfloat16)
    own_ref[...] = jnp.concatenate(
        [dk_own[h] * scale for h in range(kv_local)] + [dv_own[h] for h in range(kv_local)], axis=1)
    sel_ref[...] = jnp.concatenate(
        [dk_sel[h] * scale for h in range(kv_local)] + [dv_sel[h] for h in range(kv_local)],
        axis=1).astype(sel_ref.dtype)


def landing_kernel(incoming, own_ref, back_ref, x_ref, dk_ref, dv_ref, part_ref, total):
    half = dk_ref.shape[1]
    owners = back_ref.shape[0]
    total[...] = own_ref[...]

    def land(s, carry):
        at = pl.ds(pl.multiple_of(jnp.maximum(incoming[s], 0) * KB, KB), KB)
        total[at, :] += back_ref[s].astype(jnp.float32)
        return carry

    if owners <= 8:
        for s in range(owners):
            land(s, 0)
    else:
        lax.fori_loop(0, owners, land, 0)
    dk = total[:, :half].astype(jnp.bfloat16)
    dk_ref[...] = dk
    dv_ref[...] = total[:, half:].astype(jnp.bfloat16)
    width = part_ref.shape[2]
    part = dot_tn(dk, x_ref[...]).astype(part_ref.dtype)
    for i in range(owners):
        part_ref[i] = part[:, i * width:(i + 1) * width]


def sum_kernel(parts_ref, out_ref):
    acc = parts_ref[0].astype(jnp.float32)
    for i in range(1, parts_ref.shape[0]):
        acc = acc + parts_ref[i].astype(jnp.float32)
    out_ref[...] = acc.T


def per_device(queries, key_vectors, value_vectors, log_sums, out_grad, layer_input, chosen):
    owners = lax.axis_size("kv")
    me = lax.axis_index("kv")
    span, width = queries.shape
    half = key_vectors.shape[1]
    kv_local = half // HEAD
    group = width // half
    blocks = span // QB
    blocks_here = span // KB
    f32, bf16 = jnp.float32, jnp.bfloat16
    vmem = pl.BlockSpec(memory_space=pltpu.VMEM)
    smem = pl.BlockSpec(memory_space=pltpu.SMEM)

    ids = jnp.arange(owners, dtype=jnp.int32)
    owner_of = jnp.where(chosen >= 0, chosen // blocks_here, -1)
    matched = owner_of[:, :, None] == ids[None, None, :]
    within = (chosen % blocks_here)[:, :, None]
    wanted = jnp.max(jnp.where(matched, within, -1), axis=(0, 1))
    used = jnp.any(matched, axis=1)
    bias = jnp.repeat(jnp.where(used, 0.0, MASKED).T, KB, axis=0)

    paired = jnp.concatenate([key_vectors, value_vectors], axis=1)
    note_rows = -(-owners // (2 * half * PAD_ROWS)) * PAD_ROWS
    note = jnp.pad(wanted.astype(bf16), (0, note_rows * 2 * half - owners)).reshape(note_rows, 2 * half)
    sent = jnp.concatenate([paired, note], axis=0)
    everyone = lax.all_gather(sent, "kv", axis=0, tiled=False)
    incoming = lax.dynamic_index_in_dim(
        everyone[:, span:, :].reshape(owners, -1), me, axis=1, keepdims=False).astype(jnp.int32)
    full_input = lax.all_gather(layer_input, "tp", axis=1, tiled=True)
    sums = log_sums.reshape(blocks, QB, kv_local, group).transpose(2, 0, 3, 1).reshape(
        kv_local * blocks, group * QB)

    query_grad, own, sel = pl.pallas_call(
        attention_kernel,
        name="attention",
        out_shape=(
            jax.ShapeDtypeStruct((span, width), bf16),
            jax.ShapeDtypeStruct((span, 2 * half), f32),
            jax.ShapeDtypeStruct((owners * KB, 2 * half), bf16),
        ),
        in_specs=[smem] + [vmem] * 6,
        out_specs=(vmem,) * 3,
        scratch_shapes=[
            pltpu.VMEM((owners * KB, 2 * half), bf16),
            pltpu.VMEM((kv_local, span, HEAD), f32),
            pltpu.VMEM((kv_local, span, HEAD), f32),
            pltpu.VMEM((kv_local, owners * KB, HEAD), f32),
            pltpu.VMEM((kv_local, owners * KB, HEAD), f32),
            pltpu.VMEM((owners * KB, group * QB), f32),
            pltpu.VMEM((owners * KB, group * QB), f32),
        ],
    )(wanted, queries, out_grad, paired, everyone, sums, bias)

    back = lax.all_to_all(sel.reshape(owners, KB, 2 * half), "kv", split_axis=0, concat_axis=0, tiled=True)
    rows = full_input.shape[1] // owners
    key_grad, value_grad, parts = pl.pallas_call(
        landing_kernel,
        name="landing",
        out_shape=(
            jax.ShapeDtypeStruct((span, half), bf16),
            jax.ShapeDtypeStruct((span, half), bf16),
            jax.ShapeDtypeStruct((owners, half, rows), bf16),
        ),
        in_specs=[smem] + [vmem] * 3,
        out_specs=(vmem,) * 3,
        scratch_shapes=[pltpu.VMEM((span, 2 * half), f32)],
    )(incoming, own, back, full_input)
    parts = lax.all_to_all(parts, "kv", split_axis=0, concat_axis=0, tiled=True)
    weight_grad = pl.pallas_call(
        sum_kernel,
        name="sum_parts",
        out_shape=jax.ShapeDtypeStruct((rows, half), f32),
        in_specs=[vmem],
        out_specs=vmem,
    )(parts)
    return (query_grad, key_grad, value_grad, weight_grad)


def solution(mesh):
    placed = (P("kv", "tp"),) * 6 + (P("kv", None),)
    return jax.shard_map(
        per_device,
        mesh=mesh,
        in_specs=placed,
        out_specs=(P("kv", "tp"),) * 4,
        check_vma=False,
    )
```

```python
import math

import jax
import jax.numpy as jnp
from jax import lax
from jax.experimental import pallas as pl
from jax.experimental.pallas import tpu as pltpu
from jax.sharding import PartitionSpec as P

HEAD = 64
KB = 32
QB = 64
MASKED = -1e30


def dot_nt(a, b):
    return lax.dot_general(a, b, (((1,), (1,)), ((), ())), preferred_element_type=jnp.float32)


def dot_nn(a, b):
    return lax.dot_general(a, b, (((1,), (0,)), ((), ())), preferred_element_type=jnp.float32)


def dot_tn(a, b):
    return lax.dot_general(a, b, (((0,), (0,)), ((), ())), preferred_element_type=jnp.float32)


def pick_kernel(incoming, k_ref, v_ref, out_ref):
    half = k_ref.shape[1]

    def pick(o, carry):
        at = pl.ds(pl.multiple_of(jnp.maximum(incoming[o], 0) * KB, KB), KB)
        out_ref[o, :, :half] = k_ref[at, :]
        out_ref[o, :, half:] = v_ref[at, :]
        return carry

    loop(out_ref.shape[0], pick, 0)


def loop(count, body, init):
    if count > 8:
        return lax.fori_loop(0, count, body, init)
    for i in range(count):
        init = body(i, init)
    return init


def attention_kernel(q_ref, g_ref, k_ref, v_ref, kv_sel, sums_ref, bias_ref,
                     dq_ref, own_ref, sel_ref,
                     dk_own, dv_own, dk_sel, dv_sel, p_buf, dp_buf):
    span = q_ref.shape[0]
    half = k_ref.shape[1]
    kv_local = half // HEAD
    group = q_ref.shape[1] // half
    blocks = span // QB
    owners = kv_sel.shape[0] // KB
    scale = HEAD ** -0.5
    chunk = math.gcd(owners, 8) * KB
    chunks = owners * KB // chunk

    def over_chunks(body, init):
        if chunks == 1:
            return body(0, init)
        return lax.fori_loop(0, chunks, body, init)

    key_id = lax.broadcasted_iota(jnp.int32, (QB, group * QB), 0)
    query_id = lax.broadcasted_iota(jnp.int32, (QB, group * QB), 1) % QB
    causal = key_id <= query_id

    for h in range(kv_local):
        k_lanes = slice(h * HEAD, (h + 1) * HEAD)
        v_lanes = slice(half + h * HEAD, half + (h + 1) * HEAD)
        for b in range(blocks):
            rows = slice(b * QB, (b + 1) * QB)
            heads = [h * group + i for i in range(group)]
            qs = jnp.concatenate([q_ref[rows, i * HEAD:(i + 1) * HEAD] for i in heads], axis=0)
            gs = jnp.concatenate([g_ref[rows, i * HEAD:(i + 1) * HEAD] for i in heads], axis=0)
            sums = sums_ref[h * blocks + b:h * blocks + b + 1, :]
            n_own = (b + 1) * QB
            k_own = k_ref[:n_own, k_lanes]
            v_own = v_ref[:n_own, k_lanes]
            p_own = jnp.exp(dot_nt(k_own, qs) * scale - sums)
            last = jnp.where(causal, p_own[b * QB:, :], 0.0)
            p_own = jnp.concatenate([p_own[:b * QB, :], last], axis=0) if b else last
            dp_own = dot_nt(v_own, gs)
            p16_own = p_own.astype(jnp.bfloat16)
            delta = jnp.sum(p16_own.astype(jnp.float32) * dp_own, axis=0, keepdims=True)

            def first_pass(c, delta):
                at = pl.ds(c * chunk, chunk)
                s = dot_nt(kv_sel[at, k_lanes], qs) * scale - sums
                p = jnp.exp(s + bias_ref[at, b:b + 1])
                dp = dot_nt(kv_sel[at, v_lanes], gs)
                p_buf[at, :] = p
                dp_buf[at, :] = dp
                p16 = p.astype(jnp.bfloat16)
                dv = dot_nn(p16, gs)
                dv_sel[h, at, :] = dv if b == 0 else dv_sel[h, at, :] + dv
                return delta + jnp.sum(p16.astype(jnp.float32) * dp, axis=0, keepdims=True)

            delta = over_chunks(first_pass, delta)
            ds_own = (p_own * (dp_own - delta)).astype(jnp.bfloat16)
            dqt = dot_tn(k_own, ds_own)
            dk = dot_nn(ds_own, qs)
            dv = dot_nn(p16_own, gs)
            if b:
                dk_own[h, :b * QB, :] += dk[:b * QB]
                dv_own[h, :b * QB, :] += dv[:b * QB]
            dk_own[h, b * QB:n_own, :] = dk[b * QB:]
            dv_own[h, b * QB:n_own, :] = dv[b * QB:]

            def second_pass(c, dqt):
                at = pl.ds(c * chunk, chunk)
                ds = (p_buf[at, :] * (dp_buf[at, :] - delta)).astype(jnp.bfloat16)
                dk = dot_nn(ds, qs)
                dk_sel[h, at, :] = dk if b == 0 else dk_sel[h, at, :] + dk
                return dqt + dot_tn(kv_sel[at, k_lanes], ds)

            dqt = over_chunks(second_pass, dqt)
            dq = (dqt * scale).T
            dq = jnp.concatenate([dq[i * QB:(i + 1) * QB] for i in range(group)], axis=1)
            dq_ref[rows, h * group * HEAD:(h + 1) * group * HEAD] = dq.astype(jnp.bfloat16)
    own_ref[...] = jnp.concatenate(
        [dk_own[h] * scale for h in range(kv_local)] + [dv_own[h] for h in range(kv_local)], axis=1)
    sel_ref[...] = jnp.concatenate(
        [dk_sel[h] * scale for h in range(kv_local)] + [dv_sel[h] for h in range(kv_local)],
        axis=1).astype(sel_ref.dtype)


def landing_kernel(incoming, sources, own_ref, back_ref, *refs):
    x_refs = refs[:-4]
    dk_ref, dv_ref, part_ref, total = refs[-4:]
    half = dk_ref.shape[1]
    total[...] = own_ref[...]

    def land(s, carry):
        at = pl.ds(pl.multiple_of(jnp.maximum(incoming[s], 0) * KB, KB), KB)
        total[at, :] += back_ref[s].astype(jnp.float32)
        return carry

    loop(back_ref.shape[0], land, 0)
    dk = total[:, :half].astype(jnp.bfloat16)
    dk_ref[...] = dk
    dv_ref[...] = total[:, half:].astype(jnp.bfloat16)
    width = part_ref.shape[2]
    for r, x_ref in enumerate(x_refs):
        part = dot_tn(dk, x_ref[...]).astype(part_ref.dtype)
        each = x_ref.shape[1] // width
        for c in range(each):
            part_ref[sources[r] * each + c] = part[:, c * width:(c + 1) * width]


def sum_kernel(parts_ref, out_ref):
    acc = parts_ref[0].astype(jnp.float32)
    for i in range(1, parts_ref.shape[0]):
        acc = acc + parts_ref[i].astype(jnp.float32)
    out_ref[...] = acc.T


def per_device(queries, key_vectors, value_vectors, log_sums, out_grad, layer_input, chosen):
    owners = lax.axis_size("kv")
    span, width = queries.shape
    half = key_vectors.shape[1]
    kv_local = half // HEAD
    group = width // half
    blocks = span // QB
    blocks_here = span // KB
    f32, bf16 = jnp.float32, jnp.bfloat16
    vmem = pl.BlockSpec(memory_space=pltpu.VMEM)
    smem = pl.BlockSpec(memory_space=pltpu.SMEM)

    ids = jnp.arange(owners, dtype=jnp.int32)
    owner_of = jnp.where(chosen >= 0, chosen // blocks_here, -1)
    matched = owner_of[:, :, None] == ids[None, None, :]
    within = (chosen % blocks_here)[:, :, None]
    wanted = jnp.max(jnp.where(matched, within, -1), axis=(0, 1))
    used = jnp.any(matched, axis=1)
    bias = jnp.repeat(jnp.where(used, 0.0, MASKED).T, KB, axis=0)

    incoming = lax.all_to_all(wanted[:, None], "kv", split_axis=0, concat_axis=0, tiled=True)[:, 0]
    tp = lax.axis_size("tp")
    mine = lax.axis_index("tp")
    pieces, sources = [], []
    for d in range(tp // 2):
        turned = [(t, (t + 2 * d) % tp) for t in range(tp)]
        pieces.append(lax.ppermute(layer_input, "tp", turned) if d else layer_input)
        sources.append((mine - 2 * d) % tp)
    for d in range(tp // 2):
        pieces.append(lax.ppermute(pieces[d], "tp", [(t, t ^ 1) for t in range(tp)]))
        sources.append(((mine ^ 1) - 2 * d) % tp)
    outgoing = pl.pallas_call(
        pick_kernel,
        name="pick",
        out_shape=jax.ShapeDtypeStruct((owners, KB, 2 * half), bf16),
        in_specs=[smem, vmem, vmem],
        out_specs=vmem,
    )(incoming, key_vectors, value_vectors)
    fetched = lax.all_to_all(outgoing, "kv", split_axis=0, concat_axis=0, tiled=True)
    sums = log_sums.reshape(blocks, QB, kv_local, group).transpose(2, 0, 3, 1).reshape(
        kv_local * blocks, group * QB)

    query_grad, own, sel = pl.pallas_call(
        attention_kernel,
        name="attention",
        out_shape=(
            jax.ShapeDtypeStruct((span, width), bf16),
            jax.ShapeDtypeStruct((span, 2 * half), f32),
            jax.ShapeDtypeStruct((owners * KB, 2 * half), bf16),
        ),
        in_specs=[vmem] * 7,
        out_specs=(vmem,) * 3,
        scratch_shapes=[
            pltpu.VMEM((kv_local, span, HEAD), f32),
            pltpu.VMEM((kv_local, span, HEAD), f32),
            pltpu.VMEM((kv_local, owners * KB, HEAD), f32),
            pltpu.VMEM((kv_local, owners * KB, HEAD), f32),
            pltpu.VMEM((owners * KB, group * QB), f32),
            pltpu.VMEM((owners * KB, group * QB), f32),
        ],
    )(queries, out_grad, key_vectors, value_vectors, fetched.reshape(owners * KB, 2 * half), sums, bias)

    back = lax.all_to_all(sel.reshape(owners, KB, 2 * half), "kv", split_axis=0, concat_axis=0, tiled=True)
    rows = layer_input.shape[1] * tp // owners
    key_grad, value_grad, parts = pl.pallas_call(
        landing_kernel,
        name="landing",
        out_shape=(
            jax.ShapeDtypeStruct((span, half), bf16),
            jax.ShapeDtypeStruct((span, half), bf16),
            jax.ShapeDtypeStruct((owners, half, rows), bf16),
        ),
        in_specs=[smem] * 2 + [vmem] * (2 + tp),
        out_specs=(vmem,) * 3,
        scratch_shapes=[pltpu.VMEM((span, 2 * half), f32)],
    )(incoming, jnp.stack(sources), own, back, *pieces)
    parts = lax.all_to_all(parts, "kv", split_axis=0, concat_axis=0, tiled=True)
    weight_grad = pl.pallas_call(
        sum_kernel,
        name="sum_parts",
        out_shape=jax.ShapeDtypeStruct((rows, half), f32),
        in_specs=[vmem],
        out_specs=vmem,
    )(parts)
    return (query_grad, key_grad, value_grad, weight_grad)


def solution(mesh):
    placed = (P("kv", "tp"),) * 6 + (P("kv", None),)
    return jax.shard_map(
        per_device,
        mesh=mesh,
        in_specs=placed,
        out_specs=(P("kv", "tp"),) * 4,
        check_vma=False,
    )
```

```python
import math

import jax
import jax.numpy as jnp
from jax import lax
from jax.experimental import pallas as pl
from jax.experimental.pallas import tpu as pltpu
from jax.sharding import PartitionSpec as P

HEAD = 64
KB = 32
QB = 64
MASKED = -1e30


def dot_nt(a, b):
    return lax.dot_general(a, b, (((1,), (1,)), ((), ())), preferred_element_type=jnp.float32)


def dot_nn(a, b):
    return lax.dot_general(a, b, (((1,), (0,)), ((), ())), preferred_element_type=jnp.float32)


def dot_tn(a, b):
    return lax.dot_general(a, b, (((0,), (0,)), ((), ())), preferred_element_type=jnp.float32)


def table_kernel(chosen, wanted_ref, bias_ref):
    row = lax.broadcasted_iota(jnp.int32, wanted_ref.shape, 0)
    lane = lax.broadcasted_iota(jnp.int32, wanted_ref.shape, 1)
    blocks, entries = chosen.shape
    per_owner = blocks * QB // KB
    wanted = jnp.full(wanted_ref.shape, -1, jnp.int32)
    bias = jnp.full(wanted_ref.shape, MASKED, jnp.float32)
    for b in range(blocks):
        for j in range(entries):
            c = chosen[b, j]
            at_zero = jnp.maximum(c, 0)
            owner = jnp.where(c >= 0, at_zero // per_owner, -1)
            hit = row == owner
            wanted = jnp.where(hit, at_zero % per_owner, wanted)
            bias = jnp.where(hit & (lane == b), 0.0, bias)
    wanted_ref[...] = wanted
    bias_ref[...] = bias


def pick_kernel(incoming, k_ref, v_ref, out_ref):
    half = k_ref.shape[1]

    def pick(o, carry):
        at = pl.ds(pl.multiple_of(jnp.maximum(incoming[o, 0], 0) * KB, KB), KB)
        out_ref[o, :, :half] = k_ref[at, :]
        out_ref[o, :, half:] = v_ref[at, :]
        return carry

    loop(out_ref.shape[0], pick, 0)


def loop(count, body, init):
    if count > 8:
        return lax.fori_loop(0, count, body, init)
    for i in range(count):
        init = body(i, init)
    return init


def attention_kernel(bias, q_ref, g_ref, k_ref, v_ref, kv_sel, sums_ref,
                     dq_ref, own_ref, sel_ref,
                     dk_own, dv_own, dk_sel, dv_sel, p_buf, dp_buf):
    span = q_ref.shape[0]
    half = k_ref.shape[1]
    kv_local = half // HEAD
    group = q_ref.shape[1] // half
    blocks = span // QB
    owners = kv_sel.shape[0] // KB
    scale = HEAD ** -0.5
    chunk = math.gcd(owners, 8) * KB
    chunks = owners * KB // chunk

    def over_chunks(body, init):
        if chunks == 1:
            return body(0, init)
        return lax.fori_loop(0, chunks, body, init)

    key_id = lax.broadcasted_iota(jnp.int32, (QB, group * QB), 0)
    query_id = lax.broadcasted_iota(jnp.int32, (QB, group * QB), 1) % QB
    causal = key_id <= query_id

    for h in range(kv_local):
        k_lanes = slice(h * HEAD, (h + 1) * HEAD)
        v_lanes = slice(half + h * HEAD, half + (h + 1) * HEAD)
        for b in range(blocks):
            rows = slice(b * QB, (b + 1) * QB)
            heads = [h * group + i for i in range(group)]
            qs = jnp.concatenate([q_ref[rows, i * HEAD:(i + 1) * HEAD] for i in heads], axis=0) * jnp.bfloat16(scale)
            gs = jnp.concatenate([g_ref[rows, i * HEAD:(i + 1) * HEAD] for i in heads], axis=0)
            sums = sums_ref[h * blocks + b:h * blocks + b + 1, :]
            n_own = (b + 1) * QB
            k_own = k_ref[:n_own, k_lanes]
            v_own = v_ref[:n_own, k_lanes]
            p_own = jnp.exp(dot_nt(k_own, qs) - sums)
            last = jnp.where(causal, p_own[b * QB:, :], 0.0)
            p_own = jnp.concatenate([p_own[:b * QB, :], last], axis=0) if b else last
            dp_own = dot_nt(v_own, gs)
            p16_own = p_own.astype(jnp.bfloat16)
            delta = jnp.sum(p16_own.astype(jnp.float32) * dp_own, axis=0, keepdims=True)

            def first_pass(c, delta):
                at = pl.ds(c * chunk, chunk)
                s = dot_nt(kv_sel[at, k_lanes], qs)
                p = jnp.exp(jnp.concatenate(
                    [s[i * KB:(i + 1) * KB] + (bias[c * (chunk // KB) + i, b] - sums)
                     for i in range(chunk // KB)], axis=0))
                dp = dot_nt(kv_sel[at, v_lanes], gs)
                p_buf[at, :] = p
                dp_buf[at, :] = dp
                p16 = p.astype(jnp.bfloat16)
                dv = dot_nn(p16, gs)
                dv_sel[h, at, :] = dv if b == 0 else dv_sel[h, at, :] + dv
                return delta + jnp.sum(p16.astype(jnp.float32) * dp, axis=0, keepdims=True)

            delta = over_chunks(first_pass, delta)
            ds_own = (p_own * (dp_own - delta)).astype(jnp.bfloat16)
            dqt = dot_tn(k_own, ds_own)
            dk = dot_nn(ds_own, qs)
            dv = dot_nn(p16_own, gs)
            if b:
                dk_own[h, :b * QB, :] += dk[:b * QB]
                dv_own[h, :b * QB, :] += dv[:b * QB]
            dk_own[h, b * QB:n_own, :] = dk[b * QB:]
            dv_own[h, b * QB:n_own, :] = dv[b * QB:]

            def second_pass(c, dqt):
                at = pl.ds(c * chunk, chunk)
                ds = (p_buf[at, :] * (dp_buf[at, :] - delta)).astype(jnp.bfloat16)
                dk = dot_nn(ds, qs)
                dk_sel[h, at, :] = dk if b == 0 else dk_sel[h, at, :] + dk
                return dqt + dot_tn(kv_sel[at, k_lanes], ds)

            dqt = over_chunks(second_pass, dqt)
            dq = (dqt * scale).T
            dq = jnp.concatenate([dq[i * QB:(i + 1) * QB] for i in range(group)], axis=1)
            dq_ref[rows, h * group * HEAD:(h + 1) * group * HEAD] = dq.astype(jnp.bfloat16)
    own_ref[...] = jnp.concatenate(
        [dk_own[h] for h in range(kv_local)] + [dv_own[h] for h in range(kv_local)], axis=1)
    sel_ref[...] = jnp.concatenate(
        [dk_sel[h] for h in range(kv_local)] + [dv_sel[h] for h in range(kv_local)],
        axis=1).astype(sel_ref.dtype)


def landing_kernel(incoming, sources, own_ref, back_ref, *refs):
    x_refs = refs[:-4]
    dk_ref, dv_ref, part_ref, total = refs[-4:]
    half = dk_ref.shape[1]
    total[...] = own_ref[...]

    def land(s, carry):
        at = pl.ds(pl.multiple_of(jnp.maximum(incoming[s, 0], 0) * KB, KB), KB)
        total[at, :] += back_ref[s].astype(jnp.float32)
        return carry

    loop(back_ref.shape[0], land, 0)
    dk = total[:, :half].astype(jnp.bfloat16)
    dk_ref[...] = dk
    dv_ref[...] = total[:, half:].astype(jnp.bfloat16)
    width = part_ref.shape[2]
    for r, x_ref in enumerate(x_refs):
        part = dot_tn(dk, x_ref[...]).astype(part_ref.dtype)
        each = x_ref.shape[1] // width
        for c in range(each):
            part_ref[sources[r] * each + c] = part[:, c * width:(c + 1) * width]


def sum_kernel(parts_ref, out_ref):
    acc = parts_ref[0].astype(jnp.float32)
    for i in range(1, parts_ref.shape[0]):
        acc = acc + parts_ref[i].astype(jnp.float32)
    out_ref[...] = acc.T


def per_device(queries, key_vectors, value_vectors, log_sums, out_grad, layer_input, chosen):
    owners = lax.axis_size("kv")
    span, width = queries.shape
    half = key_vectors.shape[1]
    kv_local = half // HEAD
    group = width // half
    blocks = span // QB
    f32, bf16 = jnp.float32, jnp.bfloat16
    vmem = pl.BlockSpec(memory_space=pltpu.VMEM)
    smem = pl.BlockSpec(memory_space=pltpu.SMEM)

    wanted, bias = pl.pallas_call(
        table_kernel,
        name="tables",
        out_shape=(jax.ShapeDtypeStruct((owners, 128), jnp.int32),
                   jax.ShapeDtypeStruct((owners, 128), f32)),
        in_specs=[smem],
        out_specs=(vmem, vmem),
    )(chosen)
    incoming = lax.all_to_all(wanted, "kv", split_axis=0, concat_axis=0, tiled=True)
    tp = lax.axis_size("tp")
    mine = lax.axis_index("tp")
    pieces, sources = [], []
    for d in range(tp // 2):
        turned = [(t, (t + 2 * d) % tp) for t in range(tp)]
        pieces.append(lax.ppermute(layer_input, "tp", turned) if d else layer_input)
        sources.append((mine - 2 * d) % tp)
    for d in range(tp // 2):
        pieces.append(lax.ppermute(pieces[d], "tp", [(t, t ^ 1) for t in range(tp)]))
        sources.append(((mine ^ 1) - 2 * d) % tp)
    outgoing = pl.pallas_call(
        pick_kernel,
        name="pick",
        out_shape=jax.ShapeDtypeStruct((owners, KB, 2 * half), bf16),
        in_specs=[smem, vmem, vmem],
        out_specs=vmem,
    )(incoming, key_vectors, value_vectors)
    fetched = lax.all_to_all(outgoing, "kv", split_axis=0, concat_axis=0, tiled=True)
    sums = log_sums.reshape(blocks, QB, kv_local, group).transpose(2, 0, 3, 1).reshape(
        kv_local * blocks, group * QB)

    query_grad, own, sel = pl.pallas_call(
        attention_kernel,
        name="attention",
        out_shape=(
            jax.ShapeDtypeStruct((span, width), bf16),
            jax.ShapeDtypeStruct((span, 2 * half), f32),
            jax.ShapeDtypeStruct((owners * KB, 2 * half), bf16),
        ),
        in_specs=[smem] + [vmem] * 6,
        out_specs=(vmem,) * 3,
        scratch_shapes=[
            pltpu.VMEM((kv_local, span, HEAD), f32),
            pltpu.VMEM((kv_local, span, HEAD), f32),
            pltpu.VMEM((kv_local, owners * KB, HEAD), f32),
            pltpu.VMEM((kv_local, owners * KB, HEAD), f32),
            pltpu.VMEM((owners * KB, group * QB), f32),
            pltpu.VMEM((owners * KB, group * QB), f32),
        ],
    )(bias, queries, out_grad, key_vectors, value_vectors, fetched.reshape(owners * KB, 2 * half), sums)

    back = lax.all_to_all(sel.reshape(owners, KB, 2 * half), "kv", split_axis=0, concat_axis=0, tiled=True)
    rows = layer_input.shape[1] * tp // owners
    key_grad, value_grad, parts = pl.pallas_call(
        landing_kernel,
        name="landing",
        out_shape=(
            jax.ShapeDtypeStruct((span, half), bf16),
            jax.ShapeDtypeStruct((span, half), bf16),
            jax.ShapeDtypeStruct((owners, half, rows), bf16),
        ),
        in_specs=[smem] * 2 + [vmem] * (2 + tp),
        out_specs=(vmem,) * 3,
        scratch_shapes=[pltpu.VMEM((span, 2 * half), f32)],
    )(incoming, jnp.stack(sources), own, back, *pieces)
    parts = lax.all_to_all(parts, "kv", split_axis=0, concat_axis=0, tiled=True)
    step = 128 if rows % 128 == 0 else rows
    weight_grad = pl.pallas_call(
        sum_kernel,
        name="sum_parts",
        out_shape=jax.ShapeDtypeStruct((rows, half), f32),
        grid=(rows // step,),
        in_specs=[pl.BlockSpec((owners, half, step), lambda i: (0, 0, i))],
        out_specs=pl.BlockSpec((step, half), lambda i: (i, 0)),
    )(parts)
    return (query_grad, key_grad, value_grad, weight_grad)


def solution(mesh):
    placed = (P("kv", "tp"),) * 6 + (P("kv", None),)
    return jax.shard_map(
        per_device,
        mesh=mesh,
        in_specs=placed,
        out_specs=(P("kv", "tp"),) * 4,
        check_vma=False,
    )
```

```python
import math

import jax
import jax.numpy as jnp
from jax import lax
from jax.experimental import pallas as pl
from jax.experimental.pallas import tpu as pltpu
from jax.sharding import PartitionSpec as P

HEAD = 64
KB = 32
QB = 64
MASKED = -1e30


def dot_nt(a, b):
    return lax.dot_general(a, b, (((1,), (1,)), ((), ())), preferred_element_type=jnp.float32)


def dot_nn(a, b):
    return lax.dot_general(a, b, (((1,), (0,)), ((), ())), preferred_element_type=jnp.float32)


def dot_tn(a, b):
    return lax.dot_general(a, b, (((0,), (0,)), ((), ())), preferred_element_type=jnp.float32)


def table_kernel(chosen, wanted_ref, bias_ref):
    row = lax.broadcasted_iota(jnp.int32, wanted_ref.shape, 0)
    lane = lax.broadcasted_iota(jnp.int32, wanted_ref.shape, 1)
    blocks, entries = chosen.shape
    per_owner = blocks * QB // KB
    wanted = jnp.full(wanted_ref.shape, -1, jnp.int32)
    bias = jnp.full(wanted_ref.shape, MASKED, jnp.float32)
    for b in range(blocks):
        for j in range(entries):
            c = chosen[b, j]
            at_zero = jnp.maximum(c, 0)
            owner = jnp.where(c >= 0, at_zero // per_owner, -1)
            hit = row == owner
            seen = row == jnp.where(lane == 1, owner ^ 1, owner)
            wanted = jnp.where(seen & (c >= 0), at_zero % per_owner, wanted)
            bias = jnp.where(hit & (lane == b), 0.0, bias)
    wanted_ref[...] = wanted
    bias_ref[...] = bias


def pick_kernel(incoming, k_ref, v_ref, out_ref):
    half = k_ref.shape[1]

    def pick(o, carry):
        at = pl.ds(pl.multiple_of(jnp.maximum(incoming[o, 0], 0) * KB, KB), KB)
        out_ref[o, :, :half] = k_ref[at, :]
        out_ref[o, :, half:] = v_ref[at, :]
        return carry

    loop(out_ref.shape[0], pick, 0)


def loop(count, body, init):
    if count > 8:
        return lax.fori_loop(0, count, body, init)
    for i in range(count):
        init = body(i, init)
    return init


def attention_kernel(bias, q_ref, g_ref, k_ref, v_ref, kv_sel, sums_ref,
                     dq_ref, own_ref, own16_ref, sel_ref,
                     dk_own, dv_own, dk_sel, dv_sel, p_buf, dp_buf):
    span = q_ref.shape[0]
    half = k_ref.shape[1]
    kv_local = half // HEAD
    group = q_ref.shape[1] // half
    blocks = span // QB
    owners = kv_sel.shape[0] // KB
    scale = HEAD ** -0.5
    chunk = math.gcd(owners, 8) * KB
    chunks = owners * KB // chunk

    def over_chunks(body, init):
        if chunks == 1:
            return body(0, init)
        return lax.fori_loop(0, chunks, body, init)

    key_id = lax.broadcasted_iota(jnp.int32, (QB, group * QB), 0)
    query_id = lax.broadcasted_iota(jnp.int32, (QB, group * QB), 1) % QB
    causal = key_id <= query_id

    for h in range(kv_local):
        k_lanes = slice(h * HEAD, (h + 1) * HEAD)
        v_lanes = slice(half + h * HEAD, half + (h + 1) * HEAD)
        for b in range(blocks):
            rows = slice(b * QB, (b + 1) * QB)
            heads = [h * group + i for i in range(group)]
            qs = jnp.concatenate([q_ref[rows, i * HEAD:(i + 1) * HEAD] for i in heads], axis=0) * jnp.bfloat16(scale)
            gs = jnp.concatenate([g_ref[rows, i * HEAD:(i + 1) * HEAD] for i in heads], axis=0)
            sums = sums_ref[h * blocks + b:h * blocks + b + 1, :]
            n_own = (b + 1) * QB
            k_own = k_ref[:n_own, k_lanes]
            v_own = v_ref[:n_own, k_lanes]
            p_own = jnp.exp(dot_nt(k_own, qs) - sums)
            last = jnp.where(causal, p_own[b * QB:, :], 0.0)
            p_own = jnp.concatenate([p_own[:b * QB, :], last], axis=0) if b else last
            dp_own = dot_nt(v_own, gs)
            p16_own = p_own.astype(jnp.bfloat16)
            delta = jnp.sum(p16_own.astype(jnp.float32) * dp_own, axis=0, keepdims=True)

            def first_pass(c, delta):
                at = pl.ds(c * chunk, chunk)
                s = dot_nt(kv_sel[at, k_lanes], qs)
                p = jnp.exp(jnp.concatenate(
                    [s[i * KB:(i + 1) * KB] + (bias[c * (chunk // KB) + i, b] - sums)
                     for i in range(chunk // KB)], axis=0))
                dp = dot_nt(kv_sel[at, v_lanes], gs)
                p_buf[at, :] = p
                dp_buf[at, :] = dp
                p16 = p.astype(jnp.bfloat16)
                dv = dot_nn(p16, gs)
                dv_sel[h, at, :] = dv if b == 0 else dv_sel[h, at, :] + dv
                return delta + jnp.sum(p16.astype(jnp.float32) * dp, axis=0, keepdims=True)

            delta = over_chunks(first_pass, delta)
            ds_own = (p_own * (dp_own - delta)).astype(jnp.bfloat16)
            dqt = dot_tn(k_own, ds_own)
            dk = dot_nn(ds_own, qs)
            dv = dot_nn(p16_own, gs)
            if b:
                dk_own[h, :b * QB, :] += dk[:b * QB]
                dv_own[h, :b * QB, :] += dv[:b * QB]
            dk_own[h, b * QB:n_own, :] = dk[b * QB:]
            dv_own[h, b * QB:n_own, :] = dv[b * QB:]

            def second_pass(c, dqt):
                at = pl.ds(c * chunk, chunk)
                ds = (p_buf[at, :] * (dp_buf[at, :] - delta)).astype(jnp.bfloat16)
                dk = dot_nn(ds, qs)
                dk_sel[h, at, :] = dk if b == 0 else dk_sel[h, at, :] + dk
                return dqt + dot_tn(kv_sel[at, k_lanes], ds)

            dqt = over_chunks(second_pass, dqt)
            dq = (dqt * scale).T
            dq = jnp.concatenate([dq[i * QB:(i + 1) * QB] for i in range(group)], axis=1)
            dq_ref[rows, h * group * HEAD:(h + 1) * group * HEAD] = dq.astype(jnp.bfloat16)
    own_ref[...] = jnp.concatenate(
        [dk_own[h] for h in range(kv_local)] + [dv_own[h] for h in range(kv_local)], axis=1)
    own16_ref[...] = own_ref[:, :half].astype(own16_ref.dtype)

    def send(o, carry):
        at = pl.ds(pl.multiple_of(o * KB, KB), KB)
        dk = jnp.concatenate([dk_sel[h, at, :] for h in range(kv_local)], axis=1).astype(sel_ref.dtype)
        dv = jnp.concatenate([dv_sel[h, at, :] for h in range(kv_local)], axis=1).astype(sel_ref.dtype)
        sel_ref[o, :, :half] = dk
        sel_ref[o, :, half:2 * half] = dv
        sel_ref[o ^ 1, :, 2 * half:] = dk
        return carry

    loop(owners, send, 0)


def landing_kernel(incoming, sources, own_ref, near_ref, back_ref, *refs):
    x_refs = refs[:-4]
    dk_ref, dv_ref, part_ref, total = refs[-4:]
    half = dk_ref.shape[1]
    total[:, :2 * half] = own_ref[...]
    total[:, 2 * half:] = near_ref[...].astype(jnp.float32)

    def land(s, carry):
        at = pl.ds(pl.multiple_of(jnp.maximum(incoming[s, 0], 0) * KB, KB), KB)
        near = pl.ds(pl.multiple_of(jnp.maximum(incoming[s, 1], 0) * KB, KB), KB)
        total[at, :2 * half] += back_ref[s, :, :2 * half].astype(jnp.float32)
        total[near, 2 * half:] += back_ref[s, :, 2 * half:].astype(jnp.float32)
        return carry

    loop(back_ref.shape[0], land, 0)
    dk = total[:, :half].astype(jnp.bfloat16)
    dk_ref[...] = dk
    dv_ref[...] = total[:, half:2 * half].astype(jnp.bfloat16)
    both = jnp.concatenate([dk, total[:, 2 * half:].astype(jnp.bfloat16)], axis=0)
    width = part_ref.shape[2]
    for r, x_ref in enumerate(x_refs):
        part = dot_tn(both, x_ref[...]).astype(part_ref.dtype)
        each = x_ref.shape[1] // width
        for c in range(each):
            part_ref[sources[r] * each + c] = part[:, c * width:(c + 1) * width]


def sum_kernel(parts_ref, out_ref):
    acc = parts_ref[0].astype(jnp.float32)
    for i in range(1, parts_ref.shape[0]):
        acc = acc + parts_ref[i].astype(jnp.float32)
    out_ref[...] = acc.T


def per_device(queries, key_vectors, value_vectors, log_sums, out_grad, layer_input, chosen):
    owners = lax.axis_size("kv")
    span, width = queries.shape
    half = key_vectors.shape[1]
    kv_local = half // HEAD
    group = width // half
    blocks = span // QB
    f32, bf16 = jnp.float32, jnp.bfloat16
    vmem = pl.BlockSpec(memory_space=pltpu.VMEM)
    smem = pl.BlockSpec(memory_space=pltpu.SMEM)

    wanted, bias = pl.pallas_call(
        table_kernel,
        name="tables",
        out_shape=(jax.ShapeDtypeStruct((owners, 128), jnp.int32),
                   jax.ShapeDtypeStruct((owners, 128), f32)),
        in_specs=[smem],
        out_specs=(vmem, vmem),
    )(chosen)
    incoming = lax.all_to_all(wanted, "kv", split_axis=0, concat_axis=0, tiled=True)
    tp = lax.axis_size("tp")
    mine = lax.axis_index("tp")
    parity = lax.axis_index("kv") % 2
    swap = [(i, i ^ 1) for i in range(owners)]
    rows = layer_input.shape[1] * tp // owners
    split = layer_input.reshape(span, -1, 2, rows)
    kept, given = [lax.dynamic_index_in_dim(split, side, 2, keepdims=False).reshape(span, -1)
                   for side in (parity, 1 - parity)]
    pair_input = jnp.concatenate([kept, lax.ppermute(given, "kv", swap)], axis=0)
    pieces, sources = [], []
    for d in range(tp // 2):
        turned = [(t, (t + 2 * d) % tp) for t in range(tp)]
        pieces.append(lax.ppermute(pair_input, "tp", turned) if d else pair_input)
        sources.append((mine - 2 * d) % tp)
    for d in range(tp // 2):
        pieces.append(lax.ppermute(pieces[d], "tp", [(t, t ^ 1) for t in range(tp)]))
        sources.append(((mine ^ 1) - 2 * d) % tp)
    outgoing = pl.pallas_call(
        pick_kernel,
        name="pick",
        out_shape=jax.ShapeDtypeStruct((owners, KB, 2 * half), bf16),
        in_specs=[smem, vmem, vmem],
        out_specs=vmem,
    )(incoming, key_vectors, value_vectors)
    fetched = lax.all_to_all(outgoing, "kv", split_axis=0, concat_axis=0, tiled=True)
    sums = log_sums.reshape(blocks, QB, kv_local, group).transpose(2, 0, 3, 1).reshape(
        kv_local * blocks, group * QB)

    query_grad, own, own16, sel = pl.pallas_call(
        attention_kernel,
        name="attention",
        out_shape=(
            jax.ShapeDtypeStruct((span, width), bf16),
            jax.ShapeDtypeStruct((span, 2 * half), f32),
            jax.ShapeDtypeStruct((span, half), bf16),
            jax.ShapeDtypeStruct((owners, KB, 3 * half), bf16),
        ),
        in_specs=[smem] + [vmem] * 6,
        out_specs=(vmem,) * 4,
        scratch_shapes=[
            pltpu.VMEM((kv_local, span, HEAD), f32),
            pltpu.VMEM((kv_local, span, HEAD), f32),
            pltpu.VMEM((kv_local, owners * KB, HEAD), f32),
            pltpu.VMEM((kv_local, owners * KB, HEAD), f32),
            pltpu.VMEM((owners * KB, group * QB), f32),
            pltpu.VMEM((owners * KB, group * QB), f32),
        ],
    )(bias, queries, out_grad, key_vectors, value_vectors, fetched.reshape(owners * KB, 2 * half), sums)

    back = lax.all_to_all(sel, "kv", split_axis=0, concat_axis=0, tiled=True)
    near = lax.ppermute(own16, "kv", swap)
    key_grad, value_grad, parts = pl.pallas_call(
        landing_kernel,
        name="landing",
        out_shape=(
            jax.ShapeDtypeStruct((span, half), bf16),
            jax.ShapeDtypeStruct((span, half), bf16),
            jax.ShapeDtypeStruct((owners // 2, half, rows), bf16),
        ),
        in_specs=[smem] * 2 + [vmem] * (3 + tp),
        out_specs=(vmem,) * 3,
        scratch_shapes=[pltpu.VMEM((span, 3 * half), f32)],
    )(incoming, jnp.stack(sources), own, near, back, *pieces)
    parity_groups = [list(range(0, owners, 2)), list(range(1, owners, 2))]
    parts = lax.all_to_all(parts, "kv", split_axis=0, concat_axis=0, tiled=True,
                           axis_index_groups=parity_groups)
    weight_grad = pl.pallas_call(
        sum_kernel,
        name="sum_parts",
        out_shape=jax.ShapeDtypeStruct((rows, half), f32),
        in_specs=[vmem],
        out_specs=vmem,
    )(parts)
    return (query_grad, key_grad, value_grad, weight_grad)


def solution(mesh):
    placed = (P("kv", "tp"),) * 6 + (P("kv", None),)
    return jax.shard_map(
        per_device,
        mesh=mesh,
        in_specs=placed,
        out_specs=(P("kv", "tp"),) * 4,
        check_vma=False,
    )
```
